128 devices in a mesh: fs: 16 (over z, y), tp: 8 (over x, core).
Axes of the slice: x: 4, y: 4, z: 4, core: 2. Of those that a mesh axis runs over, the one named last changes fastest.
Arguments:
- stream: bfloat16 [16384, 1024], P(('fs', 'tp')), may hold values from -3 to 3
- mixer_out: bfloat16 [16384, 1024], P(('fs', 'tp')), may hold values from -6 to 6
- ffn_gains: float32 [4, 1024], replicated, may hold values from 0.5 to 1.5
- mixer_gain: float32 [1024], replicated, may hold values from 0.25 to 0.6
- gate_first: bfloat16 [1024, 2816], P('fs', 'tp'), may hold values from -0.1875 to 0.1875
- up_first: bfloat16 [1024, 2816], P('fs', 'tp'), may hold values from -0.1875 to 0.1875
- down_first: bfloat16 [2816, 1024], P('tp', 'fs'), may hold values from -0.109375 to 0.109375
- gate_second: bfloat16 [1024, 2816], P('fs', 'tp'), may hold values from -0.1875 to 0.1875
- up_second: bfloat16 [1024, 2816], P('fs', 'tp'), may hold values from -0.1875 to 0.1875
- down_second: bfloat16 [2816, 1024], P('tp', 'fs'), may hold values from -0.109375 to 0.109375
Outputs:
- layer_out: bfloat16 [16384, 1024], P(('fs', 'tp'))
The draws below stay inside these ranges and needn't reach their ends.
All inputs are finite; a program needn't handle non-finite values.
Results may differ from the reference program's by a relative error of at most 0.02.
Values may be sent and summed in bfloat16 or wider, within the bound.
A program may use at most 64 MiB of HBM per device.

```python
import jax
import jax.numpy as jnp
from jax import lax

D = 1024
FF = 2816
TOK_DEV = 128
TOKENS = 16384
N_FS = 16
N_TP = 8


def levels(stream_key, dims, split, smallest, largest):
    def one(axis_at, parts):
        draws = jax.random.uniform(jax.random.fold_in(jax.random.fold_in(stream_key, 6), axis_at), (parts,), jnp.float32, smallest / len(split), largest / len(split))
        return jnp.repeat(jnp.exp(draws), dims[axis_at] // parts).reshape((-1,) + (1,) * (len(dims) - axis_at - 1))

    level = one(*split[0])
    for cut in split[1:]:
        level = level * one(*cut)
    return level


def bell_draw(own_key, shape, width, reach, pieces=(), kind=jnp.bfloat16):
    loudness = levels(own_key, shape, pieces, -0.22, 0.18) if pieces else 1.0
    drawn = jax.random.normal(own_key, shape, jnp.float32) * width * loudness
    return jnp.minimum(jnp.maximum(drawn, -reach), reach).astype(kind)


def setup_inputs(seed: int = 0) -> dict:
    key_of = jax.random.split(jax.random.key(seed), 11)
    return {
        "stream": bell_draw(key_of[0], (TOKENS, D), 0.5, 3.0, ((0, 128),)),
        "mixer_out": bell_draw(key_of[1], (TOKENS, D), 1.0, 6.0, ((0, 128),)),
        "ffn_gains": jnp.clip(1.0 + 0.1 * jax.random.normal(key_of[2], (4, D), jnp.float32), 0.5, 1.5),
        "mixer_gain": jnp.clip(jax.random.uniform(key_of[3], (D,), jnp.float32, 0.25, 0.6), 0.25, 0.6),
        "gate_first": bell_draw(key_of[4], (D, FF), D ** -0.5, 0.1875, ((0, 16), (1, 8))),
        "up_first": bell_draw(key_of[5], (D, FF), D ** -0.5, 0.1875, ((0, 16), (1, 8))),
        "down_first": bell_draw(key_of[6], (FF, D), FF ** -0.5, 0.109375, ((0, 8), (1, 16))),
        "gate_second": bell_draw(key_of[7], (D, FF), D ** -0.5, 0.1875, ((0, 16), (1, 8))),
        "up_second": bell_draw(key_of[8], (D, FF), D ** -0.5, 0.1875, ((0, 16), (1, 8))),
        "down_second": bell_draw(key_of[9], (FF, D), FF ** -0.5, 0.109375, ((0, 8), (1, 16))),
    }


epsilon = 1e-06
half_weight = 0.5

def rms_rows(values, gain_row):
    widened = values.astype(jnp.float32)
    inverse_rms = lax.rsqrt(lax.optimization_barrier(jnp.mean(widened * widened, axis=-1, keepdims=True)) + epsilon)
    return (widened * inverse_rms * gain_row.astype(jnp.float32)).astype(jnp.bfloat16)

def add_branch(rows, normed_branch, factor):
    return (rows.astype(jnp.float32) + factor * normed_branch.astype(jnp.float32)).astype(jnp.bfloat16)

def half_step(rows, gain_pre, gain_post, gate_w, up_w, down_w):
    normed = rms_rows(rows, gain_pre)
    blocks = normed.reshape(N_FS, TOK_DEV * N_TP, D)

    def feed_block(row_block):
        gate_sum = jnp.dot(row_block, gate_w, preferred_element_type=jnp.float32)
        up_sum = jnp.dot(row_block, up_w, preferred_element_type=jnp.float32)
        hidden = (jax.nn.silu(gate_sum) * up_sum).astype(jnp.bfloat16)
        return jnp.dot(hidden, down_w, preferred_element_type=jnp.float32).astype(jnp.bfloat16)
    branch = lax.map(feed_block, blocks).reshape(TOKENS, D)
    return add_branch(rows, rms_rows(branch, gain_post), half_weight)

def reference(stream, mixer_out, ffn_gains, mixer_gain, gate_first, up_first, down_first, gate_second, up_second, down_second):
    after_first = half_step(stream, ffn_gains[0], ffn_gains[1], gate_first, up_first, down_first)
    mixed_in = add_branch(after_first, rms_rows(mixer_out, mixer_gain), 1.0)
    return half_step(mixed_in, ffn_gains[2], ffn_gains[3], gate_second, up_second, down_second)
```

```python
import functools

import jax
import jax.numpy as jnp
from jax import lax
from jax.experimental import pallas as pl
from jax.experimental.pallas import tpu as pltpu
from jax.sharding import PartitionSpec as P

EPS = 1e-06
F32 = jnp.float32
BF16 = jnp.bfloat16
D = 1024
TOK = 128
ROWS = 64
HID = 352
PAD = 384
CHUNKS = 4
N = TOK // CHUNKS
H = N // 2
NSEM = 512


def rms(v, gain):
    return v * lax.rsqrt(jnp.mean(v * v, axis=-1, keepdims=True) + EPS) * gain


def dot_t(a, b):
    return lax.dot_general(a, b, (((1,), (1,)), ((), ())), preferred_element_type=F32)


def kernel(
    stream,
    mixer,
    gains,
    mgain,
    g1,
    u1,
    d1,
    g2,
    u2,
    d2,
    out,
    wgu,
    wd,
    xa1,
    xa2,
    hid1,
    hid2,
    psend,
    rin,
    fin,
    mixed,
    mixn,
    ssem,
    rsem,
):
    fs = lax.axis_index("fs")
    tp = lax.axis_index("tp")
    z, y = fs // 4, fs % 4
    x, c = tp // 2, tp % 2

    def unit(dy, dz):
        return ((z + dz + 4) % 4) * 4 + (y + dy + 4) % 4

    def dev(f, t):
        return {"fs": f, "tp": t}

    yp, ym = dev(unit(1, 0), tp), dev(unit(-1, 0), tp)
    zp, zm = dev(unit(0, 1), tp), dev(unit(0, -1), tp)
    xp = dev(fs, ((x + 1) % 4) * 2 + c)
    xm = dev(fs, ((x + 3) % 4) * 2 + c)
    sib = dev(fs, x * 2 + 1 - c)

    barrier = pltpu.get_barrier_semaphore()
    for d in (yp, ym, zp, zm, xp, xm, sib):
        pl.semaphore_signal(
            barrier, inc=1, device_id=d, device_id_type=pl.DeviceIdType.MESH
        )

    me = pl.multiple_of(fs * ROWS, ROWS)
    eye = (
        lax.broadcasted_iota(jnp.int32, (ROWS, ROWS), 0)
        == lax.broadcasted_iota(jnp.int32, (ROWS, ROWS), 1)
    ).astype(BF16)
    for b, (g, u, d) in enumerate(((g1, u1, d1), (g2, u2, d2))):
        mine = pl.ds(me, ROWS)
        wgu[b, 0, mine, :] = jnp.zeros((ROWS, 2 * PAD), BF16)
        wgu[b, 0, mine, 0:HID] = g[...]
        wgu[b, 0, mine, PAD : PAD + HID] = u[...]
        wd[b, mine, 0:PAD] = jnp.zeros((ROWS, PAD), BF16)
        wd[b, mine, 0:HID] = dot_t(eye, d[...]).astype(BF16)
    xa1[0:TOK, :] = rms(stream[...].astype(F32), gains[0:1, :]).astype(BF16)
    mixn[...] = rms(mixer[...].astype(F32), mgain[...]).astype(BF16)

    pl.semaphore_wait(barrier, 7)

    count = [0]
    started = []

    def send(src, dst, to):
        i = count[0]
        count[0] += 1
        copy = pltpu.make_async_remote_copy(
            src_ref=src,
            dst_ref=dst,
            send_sem=ssem.at[i],
            recv_sem=rsem.at[i],
            device_id=to,
            device_id_type=pl.DeviceIdType.MESH,
        )
        copy.start()
        started.append(copy)
        return copy

    class Gather:
        def __init__(self, kind, b):
            self.kind, self.b, self.sib = kind, b, []

        def ref(self, dy, dz, q0, q1, slot=0):
            rows = pl.ds(pl.multiple_of(unit(dy, dz) * ROWS + q0 * 16, 16), (q1 - q0) * 16)
            if self.kind == "gu":
                return wgu.at[self.b, slot, rows, :]
            return wd.at[self.b, rows, slot * PAD : (slot + 1) * PAD]

        def go(self, dy, dz, q0, q1, to):
            r = self.ref(dy, dz, q0, q1)
            return send(r, r, to)

        def share(self, *units):
            for dy, dz in units:
                self.sib.append(
                    send(self.ref(dy, dz, 0, 4), self.ref(dy, dz, 0, 4, 1), sib)
                )

        def w0(self):
            self.a = [self.go(0, 0, 0, 4, t) for t in (yp, ym, zp, zm)]
            self.share((0, 0))

        def w1(self):
            go = self.go
            from_ym, from_yp, from_zm, from_zp = self.a
            from_ym.wait_recv()
            self.y2a = go(-1, 0, 0, 2, yp)
            self.zp = [go(-1, 0, 0, 2, zp)]
            self.zm = [go(-1, 0, 0, 2, zm)]
            from_yp.wait_recv()
            self.y2b = go(1, 0, 2, 4, ym)
            self.zp.append(go(1, 0, 0, 2, zp))
            self.zm.append(go(1, 0, 0, 2, zm))
            from_zm.wait_recv()
            self.z2a = go(0, -1, 0, 2, zp)
            self.yp = [go(0, -1, 2, 4, yp)]
            self.ym = [go(0, -1, 2, 4, ym)]
            from_zp.wait_recv()
            self.z2b = go(0, 1, 2, 4, zm)
            self.yp.append(go(0, 1, 2, 4, yp))
            self.ym.append(go(0, 1, 2, 4, ym))
            self.share((-1, 0), (1, 0), (0, -1), (0, 1))

        def w2(self):
            go = self.go
            self.y2a.wait_recv()
            self.zp.append(go(2, 0, 0, 2, zp))
            self.zm.append(go(2, 0, 0, 2, zm))
            self.z2b.wait_recv()
            self.yp.append(go(0, 2, 2, 4, yp))
            self.ym.append(go(0, 2, 2, 4, ym))
            self.rest = []
            for i, d in enumerate((-1, 1)):
                self.zp[i].wait_recv()
                self.rest.append(go(d, -1, 0, 1, zp))
                self.zm[i].wait_recv()
                self.rest.append(go(d, 1, 1, 2, zm))
                self.yp[i].wait_recv()
                self.rest.append(go(-1, d, 2, 3, yp))
                self.ym[i].wait_recv()
                self.rest.append(go(1, d, 3, 4, ym))
            self.y2b.wait_recv()
            self.z2a.wait_recv()
            self.share((2, 0), (0, 2), (-1, -1), (-1, 1), (1, -1), (1, 1))

        def w3(self):
            go = self.go
            self.zp[2].wait_recv()
            self.rest.append(go(2, -1, 0, 1, zp))
            self.zm[2].wait_recv()
            self.rest.append(go(2, 1, 1, 2, zm))
            self.yp[2].wait_recv()
            self.rest.append(go(-1, 2, 2, 3, yp))
            self.ym[2].wait_recv()
            self.rest.append(go(1, 2, 3, 4, ym))

        def w4(self):
            for r in self.rest:
                r.wait_recv()
            self.share((2, -1), (2, 1), (-1, 2), (1, 2), (2, 2))

        def done(self):
            for r in self.sib:
                r.wait_recv()

    gu1, dn1, gu2, dn2 = (
        Gather("gu", 0),
        Gather("d", 0),
        Gather("gu", 1),
        Gather("d", 1),
    )

    gu1.w0()
    top, bot = slice(0, TOK // 2), slice(TOK // 2, TOK)

    def slot(s, half):
        return xa1.at[pl.ds(s * TOK + half * (TOK // 2), TOK // 2), :]

    r0 = send(slot(0, 0), slot(3, 0), xp)
    l1 = send(slot(0, 1), slot(1, 1), xm)
    r1 = send(slot(0, 1), slot(3, 1), xp)
    l0 = send(slot(0, 0), slot(1, 0), xm)
    dn1.w0()
    gu1.w1()
    r0.wait_recv()
    rr = send(slot(3, 0), slot(2, 0), xp)
    l1.wait_recv()
    ll = send(slot(1, 1), slot(2, 1), xm)
    dn1.w1()
    gu1.w2()
    dn1.w2()
    gu1.w3()
    dn1.w3()
    gu2.w0()
    dn2.w0()
    gu1.w4()
    for t in (r1, l0, rr, ll):
        t.wait_recv()
    gu1.done()

    def hidden(b, rows, xv):
        parts = []
        for s in range(2):
            prod = jnp.dot(xv, wgu[b, s, :, :], preferred_element_type=F32)
            gate, up = prod[:, :PAD], prod[:, PAD:]
            parts.append((gate / (1.0 + jnp.exp(-gate)) * up).astype(BF16))
        return parts

    for i in range(2):
        rows = slice(i * 256, (i + 1) * 256)
        parts = hidden(0, rows, xa1[rows, :])
        for s in range(2):
            hid1[rows, s * PAD : (s + 1) * PAD] = parts[s]

    gu2.w1()
    dn1.w4()
    dn1.done()

    def project(b, k, h):
        part = dot_t(h, wd[b, :, :]).astype(BF16)
        for s in range(4):
            psend[b, k, s, :, :] = part[s * N : (s + 1) * N, :]

    rs = {}

    def half(h):
        return pl.ds(h * H, H)

    def scatter(b, k):
        p, q, f = psend.at[b, k], rin.at[b, k], fin.at[b, k]
        rs[b, k] = [
            send(p.at[2, half(0)], q.at[0], xp),
            send(p.at[2, half(1)], q.at[1], xm),
            send(p.at[1, half(1)], f.at[0, half(1)], xp),
            send(p.at[3, half(0)], f.at[1, half(0)], xm),
        ]

    def relay(b, k):
        p, f = psend.at[b, k], fin.at[b, k]
        a = rs[b, k]
        a[0].wait_recv()
        psend[b, k, 1, half(0), :] = (
            psend[b, k, 1, half(0), :].astype(F32) + rin[b, k, 0, :, :].astype(F32)
        ).astype(BF16)
        a.append(send(p.at[1, half(0)], f.at[0, half(0)], xp))
        a[1].wait_recv()
        psend[b, k, 3, half(1), :] = (
            psend[b, k, 3, half(1), :].astype(F32) + rin[b, k, 1, :, :].astype(F32)
        ).astype(BF16)
        a.append(send(p.at[3, half(1)], f.at[1, half(1)], xm))

    def collect(b, k):
        for t in rs[b, k][2:]:
            t.wait_recv()
        return (
            psend[b, k, 0, :, :].astype(F32)
            + fin[b, k, 0, :, :].astype(F32)
            + fin[b, k, 1, :, :].astype(F32)
        )

    ag = {}

    def middle(k):
        rows = slice(k * N, (k + 1) * N)
        branch = collect(0, k)
        after = (stream[rows, :].astype(F32) + 0.5 * rms(branch, gains[1:2, :])).astype(BF16)
        mix = (after.astype(F32) + mixn[rows, :].astype(F32)).astype(BF16)
        mixed[rows, :] = mix
        xa2[k, 0, :, :] = rms(mix.astype(F32), gains[2:3, :]).astype(BF16)
        a = xa2.at[k]
        ag[k] = [
            send(a.at[0, half(0)], a.at[3, half(0)], xp),
            send(a.at[0, half(1)], a.at[1, half(1)], xm),
            send(a.at[0, half(1)], a.at[3, half(1)], xp),
            send(a.at[0, half(0)], a.at[1, half(0)], xm),
        ]

    def forward(k):
        a = xa2.at[k]
        t = ag[k]
        t[0].wait_recv()
        t.append(send(a.at[3, half(0)], a.at[2, half(0)], xp))
        t[1].wait_recv()
        t.append(send(a.at[1, half(1)], a.at[2, half(1)], xm))

    def second(k):
        for t in ag[k][2:]:
            t.wait_recv()
        parts = hidden(1, None, xa2[k].reshape(4 * N, D))
        for s in range(2):
            hid2[:, s * PAD : (s + 1) * PAD] = parts[s]
        project(1, k, hid2[...])
        scatter(1, k)

    def finish(k):
        rows = slice(k * N, (k + 1) * N)
        branch = collect(1, k)
        out[rows, :] = (
            mixed[rows, :].astype(F32) + 0.5 * rms(branch, gains[3:4, :])
        ).astype(BF16)

    for k in range(CHUNKS):
        h = jnp.concatenate(
            [hid1[s * TOK + k * N : s * TOK + (k + 1) * N, :] for s in range(4)], axis=0
        )
        project(0, k, h)
        scatter(0, k)
    dn2.w1()
    gu2.w2()
    for k in range(CHUNKS):
        relay(0, k)
    dn2.w2()
    gu2.w3()
    for k in range(CHUNKS):
        middle(k)
    dn2.w3()
    for k in range(CHUNKS):
        forward(k)
    gu2.w4()
    dn2.w4()
    gu2.done()
    dn2.done()
    for k in range(CHUNKS):
        second(k)
    for k in range(CHUNKS):
        relay(1, k)
    for k in range(CHUNKS):
        finish(k)
    for t in started:
        t.wait_send()


def body(stream, mixer, gains, mgain, g1, u1, d1, g2, u2, d2):
    vmem = pl.BlockSpec(memory_space=pltpu.VMEM)
    return pl.pallas_call(
        kernel,
        out_shape=jax.ShapeDtypeStruct((TOK, D), BF16),
        in_specs=[vmem] * 10,
        out_specs=vmem,
        scratch_shapes=[
            pltpu.VMEM((2, 2, D, 2 * PAD), BF16),
            pltpu.VMEM((2, D, 2 * PAD), BF16),
            pltpu.VMEM((4 * TOK, D), BF16),
            pltpu.VMEM((CHUNKS, 4, N, D), BF16),
            pltpu.VMEM((4 * TOK, 2 * PAD), BF16),
            pltpu.VMEM((4 * N, 2 * PAD), BF16),
            pltpu.VMEM((2, CHUNKS, 4, N, D), BF16),
            pltpu.VMEM((2, CHUNKS, 2, H, D), BF16),
            pltpu.VMEM((2, CHUNKS, 2, N, D), BF16),
            pltpu.VMEM((TOK, D), BF16),
            pltpu.VMEM((TOK, D), BF16),
            pltpu.SemaphoreType.DMA((NSEM,)),
            pltpu.SemaphoreType.DMA((NSEM,)),
        ],
        compiler_params=pltpu.CompilerParams(
            collective_id=0, has_side_effects=True, vmem_limit_bytes=56 * 2**20
        ),
        name="macaron",
    )(stream, mixer, gains, mgain.reshape(1, D), g1, u1, d1, g2, u2, d2)


def solution(mesh):
    placed = (
        P(("fs", "tp"), None),
        P(("fs", "tp"), None),
        P(),
        P(),
        P("fs", "tp"),
        P("fs", "tp"),
        P("tp", "fs"),
        P("fs", "tp"),
        P("fs", "tp"),
        P("tp", "fs"),
    )
    return jax.shard_map(
        body, mesh=mesh, in_specs=placed, out_specs=P(("fs", "tp"), None), check_vma=False
    )
```

```python
import functools

import jax
import jax.numpy as jnp
from jax import lax
from jax.experimental import pallas as pl
from jax.experimental.pallas import tpu as pltpu
from jax.sharding import PartitionSpec as P

EPS = 1e-06
F32 = jnp.float32
BF16 = jnp.bfloat16
D = 1024
TOK = 128
ROWS = 64
HID = 352
PAD = 384
CHUNKS = 4
N = TOK // CHUNKS
H = N // 2
NRECV = 124
NSEND = 12


def rms(v, gain):
    return v * lax.rsqrt(jnp.mean(v * v, axis=-1, keepdims=True) + EPS) * gain


def dot_t(a, b):
    return lax.dot_general(a, b, (((1,), (1,)), ((), ())), preferred_element_type=F32)


def kernel(
    stream_in,
    mixer_in,
    gains_in,
    mgain_in,
    g1,
    u1,
    d1,
    g2,
    u2,
    d2,
    out,
    wgu,
    wd,
    xa1,
    xa2,
    hid1,
    hid2,
    psend,
    rin,
    fin,
    mixed,
    mixn,
    result,
    stream,
    mixer,
    gains,
    mgain,
    shards,
    ssem,
    rsem,
    lsem,
):
    fs = lax.axis_index("fs")
    tp = lax.axis_index("tp")
    z, y = fs // 4, fs % 4
    x, c = tp // 2, tp % 2

    def unit(dy, dz):
        return ((z + dz + 4) % 4) * 4 + (y + dy + 4) % 4

    def dev(f, t):
        return {"fs": f, "tp": t}

    yp, ym = dev(unit(1, 0), tp), dev(unit(-1, 0), tp)
    zp, zm = dev(unit(0, 1), tp), dev(unit(0, -1), tp)
    xp = dev(fs, ((x + 1) % 4) * 2 + c)
    xm = dev(fs, ((x + 3) % 4) * 2 + c)
    sib = dev(fs, x * 2 + 1 - c)

    open_scope = [None]

    def scope(name):
        if open_scope[0] is not None:
            open_scope[0].__exit__(None, None, None)
        open_scope[0] = jax.named_scope(name)
        open_scope[0].__enter__()

    barrier = pltpu.get_barrier_semaphore()
    for d in (yp, ym, zp, zm, xp, xm, sib):
        pl.semaphore_signal(
            barrier, inc=1, device_id=d, device_id_type=pl.DeviceIdType.MESH
        )

    scope("inputs")
    pairs = list(zip((g1, u1, d1, g2, u2, d2), shards))
    pairs += [(stream_in, stream), (gains_in, gains), (mgain_in, mgain), (mixer_in, mixer)]
    loads = [
        pltpu.make_async_copy(src, dst, lsem.at[i]) for i, (src, dst) in enumerate(pairs)
    ]
    for t in loads:
        t.start()
    for t in loads:
        t.wait()
    me = pl.multiple_of(fs * ROWS, ROWS)
    scope("prep")
    for b in range(2):
        g, u, d = shards[3 * b : 3 * b + 3]
        mine = pl.ds(me, ROWS)
        wgu[b, 0, mine, :] = jnp.zeros((ROWS, 2 * PAD), BF16)
        wgu[b, 0, mine, 0:HID] = g[...]
        wgu[b, 0, mine, PAD : PAD + HID] = u[...]
        wd[b, mine, 0:PAD] = jnp.zeros((ROWS, PAD), BF16)
        wd[b, mine, 0:HID] = d[...]
    xa1[0:TOK, :] = rms(stream[...].astype(F32), gains[0:1, :]).astype(BF16)

    scope("barrier")
    pl.semaphore_wait(barrier, 7)

    def remote(src, dst, to, ss, rs):
        return pltpu.make_async_remote_copy(
            src_ref=src,
            dst_ref=dst,
            send_sem=ssem.at[ss],
            recv_sem=rsem.at[rs],
            device_id=to,
            device_id_type=pl.DeviceIdType.MESH,
        )

    class Arrival:
        def __init__(self, whole=None):
            self.i, self.whole = count[0], whole
            count[0] += 1

        def wait(self):
            remote(self.whole, self.whole, sib, 0, self.i).wait_recv()

    class Sends:
        def __init__(self, whole):
            self.i, self.whole = len(groups), whole
            groups.append(self)

        def wait(self):
            remote(self.whole, self.whole, sib, self.i, 0).wait_send()

        def send(self, src, dst, to, arrival=None):
            arrival = arrival or Arrival(dst)
            remote(src, dst, to, self.i, arrival.i).start()
            return arrival

    count, groups = [0], []

    class Gather:
        def __init__(self, kind, b):
            self.kind, self.b = kind, b
            self.links = Sends(self.rows(0, 960))
            self.core = Sends(self.rows(0, D))
            self.far = Arrival(self.rows(0, 64))
            self.rest = Arrival(self.rows(0, 192))
            self.twin = Arrival(self.rows(0, D))

        def rows(self, at, size, slot=0):
            if self.kind == "gu":
                return wgu.at[self.b, slot, pl.ds(at, size), :]
            return wd.at[self.b, pl.ds(at, size), slot * PAD : (slot + 1) * PAD]

        def ref(self, dy, dz, q0, q1, slot=0):
            at = pl.multiple_of(unit(dy, dz) * ROWS + q0 * 16, 16)
            return self.rows(at, (q1 - q0) * 16, slot)

        def go(self, dy, dz, q0, q1, to, arrival=None):
            r = self.ref(dy, dz, q0, q1)
            return self.links.send(r, r, to, arrival)

        def share(self, *units):
            for dy, dz in units:
                self.core.send(
                    self.ref(dy, dz, 0, 4), self.ref(dy, dz, 0, 4, 1), sib, self.twin
                )

        def w0(self):
            self.a = [self.go(0, 0, 0, 4, t) for t in (yp, ym, zp, zm)]
            self.share((0, 0))

        def w1(self):
            go = self.go
            from_ym, from_yp, from_zm, from_zp = self.a
            from_ym.wait()
            self.y2a = go(-1, 0, 0, 2, yp)
            self.zp = [go(-1, 0, 0, 2, zp)]
            self.zm = [go(-1, 0, 0, 2, zm)]
            from_zp.wait()
            self.z2b = go(0, 1, 2, 4, zm)
            self.yp = [go(0, 1, 2, 4, yp)]
            self.ym = [go(0, 1, 2, 4, ym)]
            from_yp.wait()
            go(1, 0, 2, 4, ym, self.far)
            self.zp.append(go(1, 0, 0, 2, zp))
            self.zm.append(go(1, 0, 0, 2, zm))
            from_zm.wait()
            go(0, -1, 0, 2, zp, self.far)
            self.yp.append(go(0, -1, 2, 4, yp))
            self.ym.append(go(0, -1, 2, 4, ym))
            self.share((-1, 0), (1, 0), (0, -1), (0, 1))

        def w2(self):
            go = self.go
            self.y2a.wait()
            self.zp.append(go(2, 0, 0, 2, zp))
            self.zm.append(go(2, 0, 0, 2, zm))
            self.z2b.wait()
            self.yp.append(go(0, 2, 2, 4, yp))
            self.ym.append(go(0, 2, 2, 4, ym))
            for i, d in enumerate((-1, 1)):
                self.zp[i].wait()
                go(d, -1, 0, 1, zp, self.rest)
                self.zm[i].wait()
                go(d, 1, 1, 2, zm, self.rest)
                self.yp[i].wait()
                go(-1, -d, 2, 3, yp, self.rest)
                self.ym[i].wait()
                go(1, -d, 3, 4, ym, self.rest)
            self.share((-1, -1), (-1, 1), (1, -1), (1, 1))

        def w3(self):
            go = self.go
            self.zp[2].wait()
            go(2, -1, 0, 1, zp, self.rest)
            self.zm[2].wait()
            go(2, 1, 1, 2, zm, self.rest)
            self.yp[2].wait()
            go(-1, 2, 2, 3, yp, self.rest)
            self.ym[2].wait()
            go(1, 2, 3, 4, ym, self.rest)
            self.far.wait()
            self.share((2, 0), (0, 2))

        def w4(self):
            self.rest.wait()
            self.share((2, -1), (2, 1), (-1, 2), (1, 2), (2, 2))

        def done(self):
            self.twin.wait()

    gu1, dn1, gu2, dn2 = (
        Gather("gu", 0),
        Gather("d", 0),
        Gather("gu", 1),
        Gather("d", 1),
    )

    tok1 = Sends(xa1.at[pl.ds(0, 384), :])
    end1 = Arrival(xa1.at[pl.ds(0, 256), :])

    def slot(s, part):
        return xa1.at[pl.ds(s * TOK + part * (TOK // 2), TOK // 2), :]

    scope("w0")
    gu1.w0()
    r0 = tok1.send(slot(0, 0), slot(3, 0), xp)
    l1 = tok1.send(slot(0, 1), slot(1, 1), xm)
    tok1.send(slot(0, 1), slot(3, 1), xp, end1)
    tok1.send(slot(0, 0), slot(1, 0), xm, end1)
    dn1.w0()
    scope("gu1_w1")
    gu1.w1()
    scope("ag1_relay")
    r0.wait()
    tok1.send(slot(3, 0), slot(2, 0), xp, end1)
    l1.wait()
    tok1.send(slot(1, 1), slot(2, 1), xm, end1)
    scope("gu1_w2")
    gu1.w2()
    scope("dn1_w1")
    dn1.w1()
    scope("gu1_w3")
    gu1.w3()
    scope("dn1_w2")
    dn1.w2()
    scope("gu1_w4")
    gu1.w4()
    scope("dn1_w3")
    dn1.w3()
    gu2.w0()
    dn2.w0()
    scope("mix")
    mixn[...] = rms(mixer[...].astype(F32), mgain[...]).astype(BF16)
    scope("ag1_end")
    end1.wait()
    scope("gu1_done")
    gu1.done()

    def hidden(b, rows, xv):
        parts = []
        for s in range(2):
            prod = jnp.dot(xv, wgu[b, s, :, :], preferred_element_type=F32)
            gate, up = prod[:, :PAD], prod[:, PAD:]
            parts.append((gate / (1.0 + jnp.exp(-gate)) * up).astype(BF16))
        return parts

    for i in range(2):
        scope(f"hidden1_{i}")
        rows = slice(i * 256, (i + 1) * 256)
        parts = hidden(0, rows, xa1[rows, :])
        for s in range(2):
            hid1[rows, s * PAD : (s + 1) * PAD] = parts[s]
    scope("dn1_w4")
    dn1.w4()
    scope("dn1_done")
    dn1.done()

    def project(b, k, h):
        part = dot_t(h, wd[b, :, :]).astype(BF16)
        for s in range(4):
            psend[b, k, s, :, :] = part[s * N : (s + 1) * N, :]

    rs, ag = {}, {}
    tok2 = Sends(xa2.at[pl.ds(0, CHUNKS * 3 // 4)])
    part = [Sends(psend.at[b, pl.ds(0, CHUNKS * 3 // 4)]) for b in range(2)]

    def half(h):
        return pl.ds(h * H, H)

    def scatter(b, k):
        p, q, f = psend.at[b, k], rin.at[b, k], fin.at[b, k]
        end = Arrival(f)
        rs[b, k] = (
            part[b].send(p.at[2, half(0)], q.at[0], xp),
            part[b].send(p.at[2, half(1)], q.at[1], xm),
            end,
        )
        part[b].send(p.at[1, half(1)], f.at[0, half(1)], xp, end)
        part[b].send(p.at[3, half(0)], f.at[1, half(0)], xm, end)

    def relay(b, k):
        p, f = psend.at[b, k], fin.at[b, k]
        first, last, end = rs[b, k]
        for i, (t, s, to) in enumerate(((first, 1, xp), (last, 3, xm))):
            t.wait()
            psend[b, k, s, half(i), :] = (
                psend[b, k, s, half(i), :].astype(F32) + rin[b, k, i, :, :].astype(F32)
            ).astype(BF16)
            part[b].send(p.at[s, half(i)], f.at[i, half(i)], to, end)

    def collect(b, k):
        rs[b, k][2].wait()
        return (
            psend[b, k, 0, :, :].astype(F32)
            + fin[b, k, 0, :, :].astype(F32)
            + fin[b, k, 1, :, :].astype(F32)
        )

    def middle(k):
        rows = slice(k * N, (k + 1) * N)
        branch = collect(0, k)
        after = (stream[rows, :].astype(F32) + 0.5 * rms(branch, gains[1:2, :])).astype(BF16)
        mix = (after.astype(F32) + mixn[rows, :].astype(F32)).astype(BF16)
        mixed[rows, :] = mix
        xa2[k, 0, :, :] = rms(mix.astype(F32), gains[2:3, :]).astype(BF16)
        a = xa2.at[k]
        end = Arrival(a.at[pl.ds(0, 2)])
        ag[k] = (
            tok2.send(a.at[0, half(0)], a.at[3, half(0)], xp),
            tok2.send(a.at[0, half(1)], a.at[1, half(1)], xm),
            end,
        )
        tok2.send(a.at[0, half(1)], a.at[3, half(1)], xp, end)
        tok2.send(a.at[0, half(0)], a.at[1, half(0)], xm, end)

    def forward(k):
        a = xa2.at[k]
        first, last, end = ag[k]
        first.wait()
        tok2.send(a.at[3, half(0)], a.at[2, half(0)], xp, end)
        last.wait()
        tok2.send(a.at[1, half(1)], a.at[2, half(1)], xm, end)

    def second(k):
        ag[k][2].wait()
        parts = hidden(1, None, xa2[k].reshape(4 * N, D))
        for s in range(2):
            hid2[:, s * PAD : (s + 1) * PAD] = parts[s]
        project(1, k, hid2[...])
        scatter(1, k)

    def finish(k):
        rows = slice(k * N, (k + 1) * N)
        branch = collect(1, k)
        result[rows, :] = (
            mixed[rows, :].astype(F32) + 0.5 * rms(branch, gains[3:4, :])
        ).astype(BF16)
        copy = pltpu.make_async_copy(result.at[rows, :], out.at[rows, :], lsem.at[k])
        copy.start()
        return copy

    def first(k):
        h = jnp.concatenate(
            [hid1[s * TOK + k * N : s * TOK + (k + 1) * N, :] for s in range(4)], axis=0
        )
        project(0, k, h)
        scatter(0, k)

    def step(name, work, *at):
        scope("_".join([name] + [str(i) for i in at]))
        return work(*at)

    step("first", first, 0)
    step("first", first, 1)
    step("gu2_w1", gu2.w1)
    step("first", first, 2)
    step("first", first, 3)
    step("dn2_w1", dn2.w1)
    step("relay1", relay, 0, 0)
    step("relay1", relay, 0, 1)
    step("gu2_w2", gu2.w2)
    step("relay1", relay, 0, 2)
    step("dn2_w2", dn2.w2)
    step("relay1", relay, 0, 3)
    step("middle", middle, 0)
    step("gu2_w3", gu2.w3)
    step("middle", middle, 1)
    step("dn2_w3", dn2.w3)
    step("middle", middle, 2)
    step("middle", middle, 3)
    step("gu2_w4", gu2.w4)
    step("forward", forward, 0)
    step("dn2_w4", dn2.w4)
    for k in range(1, CHUNKS):
        step("forward", forward, k)
    step("gu2_done", gu2.done)
    step("dn2_done", dn2.done)
    for k in range(CHUNKS):
        step("second", second, k)
    for k in range(CHUNKS):
        step("relay2", relay, 1, k)
    copies = [step("finish", finish, k) for k in range(CHUNKS)]
    scope("sends")
    for t in groups:
        t.wait()
    for t in copies:
        t.wait()
    open_scope[0].__exit__(None, None, None)
    assert count[0] <= NRECV and len(groups) <= NSEND, (count, len(groups))


def body(stream, mixer, gains, mgain, g1, u1, d1, g2, u2, d2):
    hbm = pl.BlockSpec(memory_space=pltpu.HBM)
    return pl.pallas_call(
        kernel,
        out_shape=jax.ShapeDtypeStruct((TOK, D), BF16),
        in_specs=[hbm] * 10,
        out_specs=hbm,
        scratch_shapes=[
            pltpu.VMEM((2, 2, D, 2 * PAD), BF16),
            pltpu.VMEM((2, D, 2 * PAD), BF16),
            pltpu.VMEM((4 * TOK, D), BF16),
            pltpu.VMEM((CHUNKS, 4, N, D), BF16),
            pltpu.VMEM((4 * TOK, 2 * PAD), BF16),
            pltpu.VMEM((4 * N, 2 * PAD), BF16),
            pltpu.VMEM((2, CHUNKS, 4, N, D), BF16),
            pltpu.VMEM((2, CHUNKS, 2, H, D), BF16),
            pltpu.VMEM((2, CHUNKS, 2, N, D), BF16),
            pltpu.VMEM((TOK, D), BF16),
            pltpu.VMEM((TOK, D), BF16),
            pltpu.VMEM((TOK, D), BF16),
            pltpu.VMEM((TOK, D), BF16),
            pltpu.VMEM((TOK, D), BF16),
            pltpu.VMEM((4, D), F32),
            pltpu.VMEM((1, D), F32),
            [pltpu.VMEM((ROWS, HID), BF16)] * 6,
            pltpu.SemaphoreType.DMA((NSEND,)),
            pltpu.SemaphoreType.DMA((NRECV,)),
            pltpu.SemaphoreType.DMA((10,)),
        ],
        compiler_params=pltpu.CompilerParams(
            collective_id=0, has_side_effects=True, vmem_limit_bytes=57000000
        ),
        name="macaron",
    )(stream, mixer, gains, mgain.reshape(1, D), g1, u1, d1.T, g2, u2, d2.T)


def solution(mesh):
    placed = (
        P(("fs", "tp"), None),
        P(("fs", "tp"), None),
        P(),
        P(),
        P("fs", "tp"),
        P("fs", "tp"),
        P("tp", "fs"),
        P("fs", "tp"),
        P("fs", "tp"),
        P("tp", "fs"),
    )
    return jax.shard_map(
        body, mesh=mesh, in_specs=placed, out_specs=P(("fs", "tp"), None), check_vma=False
    )
```
